32 devices in a mesh: sp: 8 (over z, y), tp: 4 (over x, core).
Axes of the slice: x: 2, y: 2, z: 4, core: 2. Of those that a mesh axis runs over, the one named last changes fastest.
Arguments:
- latent: bfloat16 [1024, 2048], P(('sp', 'tp')), may hold values from -6 to 6
- context: bfloat16 [512, 2048], replicated, may hold values from -6 to 6
- condition: float32 [2048], replicated, may hold values from -6 to 6
- context_condition: float32 [2048], replicated, may hold values from -6 to 6
- modulation_weight: bfloat16 [2048, 3, 2048], P('sp', None, 'tp'), may hold values from -0.25 to 0.25
- norm_gain: float32 [2048], replicated, may hold values from 0.1 to 1.9
- gate_weight: bfloat16 [2048, 1024], P(None, 'tp'), may hold values from -0.125 to 0.125
- value_weight: bfloat16 [2048, 1024], P(None, 'tp'), may hold values from -0.125 to 0.125
- write_weight: bfloat16 [2048, 512], P(None, 'tp'), may hold values from -0.125 to 0.125
- read_weight: bfloat16 [2048, 512], P(None, 'tp'), may hold values from -0.125 to 0.125
- step_weight: bfloat16 [2048, 2, 16], replicated, may hold values from -0.125 to 0.125
- value_taps: bfloat16 [3, 1024], P(None, 'tp'), may hold values from -3.5 to 3.5
- map_taps: bfloat16 [3, 2, 512], P(None, None, 'tp'), may hold values from -3.5 to 3.5
- decay_rate: float32 [2, 16], replicated, may hold values from 1e-06 to 0.06
- decay_jump: float32 [2, 16, 1024], P(None, 'tp', 'sp'), may hold values from -2.76 to 0
- skip_gain: float32 [16], replicated, may hold values from 1 to 16
- group_gain: float32 [1024], P('tp'), may hold values from 0.1 to 1.9
- output_weight: bfloat16 [1024, 2048], P('tp'), may hold values from -0.1875 to 0.1875
- post_gain: float32 [2048], replicated, may hold values from 0.1 to 1.9
Outputs:
- updated: bfloat16 [1024, 2048], P(('sp', 'tp'))
The draws below stay inside these ranges and needn't reach their ends.
All inputs are finite; a program needn't handle non-finite values.
Results may differ from the reference program's by a relative error of at most 0.014.
Values may be sent and summed in bfloat16 or wider, within the bound.
A program may use at most 64 MiB of HBM per device.

```python
import math
import jax
import jax.numpy as jnp
from jax import lax

D = 2048
HEADS = 16
HEAD_DIM = 64
GROUPS = 8
STATE = 64
SPAN = 128
CTX = 512
INNER = 1024
TOKENS = 1024
N_TP = 4


def draw_decay_rate(key, part):
    pick_key, value_key = jax.random.split(jax.random.fold_in(key, 11))
    fast_heads = jax.random.randint(pick_key, (2, HEADS), 0, 2) == 1
    spread = jax.random.uniform(value_key, (2, HEADS), jnp.float32)
    slow_rate = jnp.exp(jnp.log(1e-06) + spread * (jnp.log(6e-05) - jnp.log(1e-06)))
    fast_rate = jnp.exp(jnp.log(0.02) + spread * (jnp.log(0.06) - jnp.log(0.02)))
    return jnp.where(fast_heads, fast_rate, slow_rate)


def draw_decay_jump(key, part):
    place_key, depth_key = jax.random.split(jax.random.fold_in(key, 23))
    places = jax.random.randint(place_key, (2, HEADS, 4), 0, TOKENS)
    depths = jax.random.uniform(depth_key, (2, HEADS, 4), jnp.float32, 0.22, 0.69)
    positions = jnp.arange(TOKENS, dtype=jnp.int32)
    hits = (positions[None, None, None, :] == places[..., None]).astype(jnp.float32)
    return -jnp.sum(hits * depths[..., None], axis=2)


def strengthened(result, key, source, target, parts, factor):
    def block_of(axis_at):
        return (jnp.arange(result.shape[axis_at]) // (result.shape[axis_at] // parts)).reshape((-1,) + (1,) * (result.ndim - 1 - axis_at))

    one_side = jax.random.permutation(key, parts)[block_of(target)]
    far = (block_of(target) + parts // 2) % parts
    return jnp.where((block_of(source) == one_side) | (block_of(source) == far), factor * result, result)


def level_of(own_key, extent, cuts, smallest, top_value):
    factor_of, own = 1.0, jax.random.fold_in(own_key, 6)
    for position, shards_of in cuts:
        heights = jnp.exp(jax.random.uniform(jax.random.fold_in(own, position), (shards_of,), jnp.float32, smallest / len(cuts), top_value / len(cuts)))
        factor_of = factor_of * jnp.repeat(heights, extent[position] // shards_of).reshape([-1 if axis == position else 1 for axis in range(len(extent))])
    return factor_of


def scatter_about(own_key, shape, scale, limit, pieces=(), kind=jnp.bfloat16):
    entries = scale * jax.random.normal(own_key, shape, jnp.float32)
    if pieces:
        entries = entries * level_of(own_key, shape, pieces, -0.22, 0.18)
    return jnp.clip(entries, -limit, limit).astype(kind)


def gaussian_with(stream_key, dims, scale, limit, cuts, heavy, held_as=jnp.bfloat16):
    drawn = scale * jax.random.normal(stream_key, dims, jnp.float32)
    if cuts:
        drawn = drawn * level_of(stream_key, dims, cuts, -0.22, 0.18)
    return jnp.clip(strengthened(drawn, jax.random.fold_in(stream_key, 3), *heavy), -limit, limit).astype(held_as)


def setup_inputs(seed: int = 0) -> dict:
    streams_of = jax.random.split(jax.random.key(seed), 20)
    latent = scatter_about(streams_of[0], (TOKENS, D), 1.0, 6.0, ((0, 32),))
    context = scatter_about(streams_of[1], (CTX, D), 1.0, 6.0)
    condition = scatter_about(streams_of[2], (D,), 1.0, 6.0, (), jnp.float32)
    context_condition = scatter_about(streams_of[3], (D,), 1.0, 6.0, (), jnp.float32)
    modulation_weight = gaussian_with(streams_of[4], (D, 3, D), (D // 2) ** -0.5, 0.25, ((0, 8), (2, 4)), (0, 2, 8, 2.0))
    norm_gain = jnp.clip(1.0 + 0.18 * jax.random.normal(streams_of[5], (D,), jnp.float32), 0.1, 1.9)
    gate_weight = scatter_about(streams_of[6], (D, INNER), D ** -0.5, 0.125, ((1, 4),))
    value_weight = scatter_about(streams_of[7], (D, INNER), D ** -0.5, 0.125, ((1, 4),))
    write_weight = scatter_about(streams_of[8], (D, GROUPS * STATE), D ** -0.5, 0.125, ((1, 4),))
    read_weight = scatter_about(streams_of[9], (D, GROUPS * STATE), D ** -0.5, 0.125, ((1, 4),))
    step_weight = scatter_about(streams_of[10], (D, 2, HEADS), D ** -0.5, 0.125)
    value_taps = scatter_about(streams_of[11], (3, INNER), 3 ** -0.5, 3.5, ((1, 4),))
    map_taps = scatter_about(streams_of[12], (3, 2, GROUPS * STATE), 3 ** -0.5, 3.5, ((2, 4),))
    decay_rate = draw_decay_rate(jax.random.fold_in(streams_of[19], 71), 0)
    decay_jump = draw_decay_jump(jax.random.fold_in(streams_of[19], 71), 0)
    skip_gain = jnp.clip(jnp.exp(jax.random.uniform(streams_of[15], (HEADS,), jnp.float32, math.log(1.0), math.log(16.0))), 1.0, 16.0)
    group_gain = jnp.clip(1.0 + 0.18 * jax.random.normal(streams_of[16], (INNER,), jnp.float32), 0.1, 1.9)
    output_weight = scatter_about(streams_of[17], (INNER, D), INNER ** -0.5, 0.1875, ((0, 4),))
    post_gain = jnp.clip(1.0 + 0.18 * jax.random.normal(streams_of[18], (D,), jnp.float32), 0.1, 1.9)
    return dict(latent=latent, context=context, condition=condition, context_condition=context_condition, modulation_weight=modulation_weight, norm_gain=norm_gain, gate_weight=gate_weight, value_weight=value_weight, write_weight=write_weight, read_weight=read_weight, step_weight=step_weight, value_taps=value_taps, map_taps=map_taps, decay_rate=decay_rate, decay_jump=decay_jump, skip_gain=skip_gain, group_gain=group_gain, output_weight=output_weight, post_gain=post_gain)


EPSILON = 1e-06
HIGHEST = lax.Precision.HIGHEST

def modulated_norm(row_block, gain_vec, shift_vec, scale_vec):
    widened = row_block.astype(jnp.float32)
    normed = widened * lax.rsqrt(lax.optimization_barrier(jnp.mean(widened * widened, axis=-1, keepdims=True)) + EPSILON)
    return (normed * gain_vec * (1.0 + scale_vec) + shift_vec).astype(jnp.bfloat16)

def short_conv(padded, conv_taps):
    length = padded.shape[0] - 2
    widened = padded.astype(jnp.float32)
    weights = conv_taps.astype(jnp.float32)
    summed = weights[0] * widened[:length] + weights[1] * widened[1:length + 1] + weights[2] * widened[2:]
    return jax.nn.silu(summed)

def zero_rim(tensor):
    return jnp.pad(tensor, ((1, 1), (0, 0)))

def project(row_block, weight):
    return jnp.dot(row_block, weight, preferred_element_type=jnp.float32).astype(jnp.bfloat16)

def flip_rows(tensor, direction):
    if direction == 1:
        return jnp.flip(tensor, axis=0)
    return tensor

def sweep(inputs, step_sizes, log_decay, write_maps, read_maps, start_state):
    length, head_count, head_width = inputs.shape
    blocks = length // SPAN
    lower_mask = (jnp.arange(SPAN)[:, None] >= jnp.arange(SPAN)[None, :])[:, :, None]

    def cut_blocks(tensor):
        return tensor.reshape((blocks, SPAN) + tensor.shape[1:])

    def advance(carry_state, block_data):
        value_block, size_block, decay_block, write_block, read_block = block_data
        within = jnp.cumsum(decay_block, axis=0)
        weighted = value_block * size_block[:, :, None]
        log_gaps = jnp.where(lower_mask, within[:, None, :] - within[None, :, :], 0.0)
        fading = jnp.where(lower_mask, jnp.exp(log_gaps), 0.0)
        scores = jnp.einsum('ihn,jhn->ijh', read_block, write_block, precision=HIGHEST) * fading
        inner_term = jnp.einsum('ijh,jhp->ihp', scores, weighted, precision=HIGHEST)
        carried = jnp.einsum('ihn,hpn->ihp', read_block * jnp.exp(within)[:, :, None], carry_state, precision=HIGHEST)
        block_total = within[-1]
        fresh_state = jnp.einsum('jhn,jhp->hpn', write_block * jnp.exp(block_total[None, :] - within)[:, :, None], weighted, precision=HIGHEST)
        return (jnp.exp(block_total)[:, None, None] * carry_state + fresh_state, inner_term + carried)
    final_state, outputs = lax.scan(advance, start_state, (cut_blocks(inputs), cut_blocks(step_sizes), cut_blocks(log_decay), cut_blocks(write_maps), cut_blocks(read_maps)))
    return (outputs.reshape(length, head_count, head_width), final_state)

def reference(latent, context, condition, context_condition, modulation_weight, norm_gain, gate_weight, value_weight, write_weight, read_weight, step_weight, value_taps, map_taps, decay_rate, decay_jump, skip_gain, group_gain, output_weight, post_gain):
    conditions = jax.nn.silu(jnp.stack([condition, context_condition]))
    modulation = jnp.einsum('sd,dkc->skc', conditions, modulation_weight.astype(jnp.float32), precision=HIGHEST)
    hidden = modulated_norm(latent, norm_gain, modulation[0, 0], modulation[0, 1])
    context_hidden = modulated_norm(context, norm_gain, modulation[1, 0], modulation[1, 1])
    step_matrix = step_weight.reshape(D, 2 * HEADS)
    gate_linear = project(hidden, gate_weight)
    step_linear = project(hidden, step_matrix).reshape(TOKENS, 2, HEADS)
    repeat_count = HEADS // GROUPS
    latent_values = short_conv(zero_rim(project(hidden, value_weight)), value_taps).reshape(TOKENS, HEADS, HEAD_DIM)
    latent_write = short_conv(zero_rim(project(hidden, write_weight)), map_taps[:, 0]).reshape(TOKENS, GROUPS, STATE)
    latent_read = short_conv(zero_rim(project(hidden, read_weight)), map_taps[:, 1]).reshape(TOKENS, GROUPS, STATE)
    latent_write = jnp.repeat(latent_write, repeat_count, axis=1)
    latent_read = jnp.repeat(latent_read, repeat_count, axis=1)
    context_values = short_conv(zero_rim(project(context_hidden, value_weight)), value_taps).reshape(CTX, HEADS, HEAD_DIM)
    context_write = short_conv(zero_rim(project(context_hidden, write_weight)), map_taps[:, 0]).reshape(CTX, GROUPS, STATE)
    context_write = jnp.repeat(context_write, repeat_count, axis=1)
    context_step = project(context_hidden, step_matrix).reshape(CTX, 2, HEADS)
    mixer_sum = skip_gain[None, :, None] * latent_values
    zero_state = jnp.zeros((HEADS, HEAD_DIM, STATE), jnp.float32)
    for direction in range(2):
        rate_head = decay_rate[direction]
        latent_size = jax.nn.softplus(step_linear[:, direction].astype(jnp.float32))
        latent_decay = -latent_size * rate_head[None, :] + decay_jump[direction].T
        context_size = jax.nn.softplus(context_step[:, direction].astype(jnp.float32))
        context_decay = -context_size * rate_head[None, :]
        unused_rows, context_state = sweep(flip_rows(context_values, direction), flip_rows(context_size, direction), flip_rows(context_decay, direction), flip_rows(context_write, direction), flip_rows(context_write, direction), zero_state)
        swept_rows, unused_state = sweep(flip_rows(latent_values, direction), flip_rows(latent_size, direction), flip_rows(latent_decay, direction), flip_rows(latent_write, direction), flip_rows(latent_read, direction), context_state)
        mixer_sum = mixer_sum + flip_rows(swept_rows, direction)
    gated_rows = mixer_sum.reshape(TOKENS, INNER) * jax.nn.silu(gate_linear.astype(jnp.float32))
    grouped = gated_rows.reshape(TOKENS, GROUPS, INNER // GROUPS)
    grouped = grouped * lax.rsqrt(lax.optimization_barrier(jnp.mean(grouped * grouped, axis=-1, keepdims=True)) + EPSILON) * group_gain.reshape(GROUPS, INNER // GROUPS)
    gated_rows = grouped.reshape(TOKENS, INNER).astype(jnp.bfloat16)
    share = INNER // N_TP
    mixed_rows = jnp.zeros((TOKENS, D), jnp.float32)
    for piece in range(N_TP):
        partial_value = jnp.dot(gated_rows[:, piece * share:(piece + 1) * share], output_weight[piece * share:(piece + 1) * share], preferred_element_type=jnp.float32)
        mixed_rows = mixed_rows + lax.optimization_barrier(partial_value.astype(jnp.bfloat16)).astype(jnp.float32)
    normed_out = mixed_rows * lax.rsqrt(lax.optimization_barrier(jnp.mean(mixed_rows * mixed_rows, axis=-1, keepdims=True)) + EPSILON) * post_gain
    return (latent.astype(jnp.float32) + modulation[0, 2] * normed_out).astype(jnp.bfloat16)
```

```python
import functools

import jax
import jax.numpy as jnp
from jax import lax
from jax.experimental import pallas as pl
from jax.experimental.pallas import tpu as pltpu
from jax.sharding import PartitionSpec as P

HEAD_DIM = 64
STATE = 64
EPSILON = 1e-06
HIGHEST = lax.Precision.HIGHEST
MESH = pl.DeviceIdType.MESH
EDGE = 16
CHUNK = 128
F32 = jnp.float32
BF16 = jnp.bfloat16


def silu(x):
    return x / (1.0 + jnp.exp(-x))


def softplus(x):
    return jnp.maximum(x, 0.0) + jnp.log1p(jnp.exp(-jnp.abs(x)))


def mask_of(shape, rule):
    rows = lax.broadcasted_iota(jnp.int32, shape, 0)
    cols = lax.broadcasted_iota(jnp.int32, shape, 1)
    return rule(rows, cols)


def tri_of(size, rule):
    return jnp.where(mask_of((size, size), rule), 1.0, 0.0).astype(F32)


def dot32(a, b):
    return jnp.dot(a, b, precision=HIGHEST, preferred_element_type=F32)


def dotf(a, b):
    return jnp.dot(a, b, preferred_element_type=F32)


def dot_nt(a, b):
    return lax.dot_general(a, b, (((1,), (1,)), ((), ())), preferred_element_type=F32)


def columns_of(rows8):
    have = rows8.shape[0]
    pad = jnp.zeros((CHUNK - have, CHUNK), F32)
    return jnp.concatenate([rows8, pad], axis=0).T


def stats_pass(src, dst, count):
    @pl.loop(0, count // 16)
    def _(i):
        at = pl.ds(pl.multiple_of(i * 16, 16), 16)
        x = src[at, :].astype(F32)
        inv = lax.rsqrt(jnp.mean(x * x, axis=-1, keepdims=True) + EPSILON)
        dst[at, :] = jnp.broadcast_to(inv, (16, 128))


def norm_pass(src, stat, dst, src_at, dst_at, count, gain, shift):
    lanes = src.shape[1] // 128

    @pl.loop(0, count // 16)
    def _(i):
        at = pl.ds(pl.multiple_of(src_at + i * 16, 16), 16)
        to = pl.ds(pl.multiple_of(dst_at + i * 16, 16), 16)
        inv = jnp.concatenate([stat[at, :]] * lanes, axis=1)
        dst[to, :] = (src[at, :].astype(F32) * inv * gain + shift).astype(BF16)


def kernel(
    part, latent, context_hbm, norm_gain, post_gain, gate_hbm, value_hbm, write_hbm, read_hbm,
    step, taps, rate, jump, skip, group_gain, output_hbm,
    out,
    context, gate_w, value_w, write_w, read_w, output_w,
    xbuf, xstat, cstat, hbuf, chid, ubuf, ucbuf, cstep,
    part_a, modbuf, stbuf, strecv, obuf, rbuf, state_c,
    load_sem, own_sem, xs_sem, xr_sem, hs_sem, hr_sem, as_sem, ar_sem, bs_sem, br_sem,
    ss_sem, sr_sem, os_sem, or_sem,
    *, n_sp, n_tp,
):
    sp, tp = lax.axis_index("sp"), lax.axis_index("tp")
    rows = latent.shape[0]
    tokens = n_tp * rows
    width = latent.shape[1]
    vwidth = value_w.shape[1]
    mwidth = write_w.shape[1]
    groups = mwidth // STATE
    heads = vwidth // HEAD_DIM
    per = heads // groups
    gwidth = vwidth // groups
    ctx = context.shape[0]
    col_chunks = obuf.shape[0]
    cwidth = obuf.shape[3]

    loads = [
        pltpu.make_async_copy(s, d, load_sem.at[i])
        for i, (s, d) in enumerate(
            (
                (context_hbm, context), (value_hbm, value_w), (write_hbm, write_w),
                (read_hbm, read_w), (gate_hbm, gate_w), (output_hbm, output_w),
            )
        )
    ]
    own_x = pltpu.make_async_copy(
        latent, xbuf.at[pl.ds(pl.multiple_of(EDGE + tp * rows, 16), rows)], own_sem
    )
    own_x.start()
    for c in loads:
        c.start()

    barrier = pltpu.get_barrier_semaphore()

    @pl.loop(1, n_sp)
    def _(r):
        pl.semaphore_signal(barrier, inc=1, device_id={"sp": lax.rem(sp + r, n_sp)}, device_id_type=MESH)

    for r in range(1, n_tp):
        pl.semaphore_signal(barrier, inc=1, device_id={"tp": lax.rem(tp + r, n_tp)}, device_id_type=MESH)
    pl.semaphore_wait(barrier, n_sp - 1 + n_tp - 1)

    def remote(src, dst, s, r, **where):
        return pltpu.make_async_remote_copy(
            src_ref=src, dst_ref=dst, send_sem=s, recv_sem=r, device_id=where, device_id_type=MESH
        )

    def send_a(r):
        peer = lax.rem(sp + r, n_sp)
        return remote(part, part_a.at[sp], as_sem.at[r], ar_sem.at[sp], sp=peer)

    def recv_a(r):
        peer = lax.rem(sp + r, n_sp)
        return remote(part, part_a.at[peer], as_sem.at[r], ar_sem.at[peer], sp=peer)

    @pl.loop(1, n_sp)
    def _(r):
        send_a(r).start()

    def x_rows(t):
        return xbuf.at[pl.ds(pl.multiple_of(EDGE + t * rows, 16), rows)]

    def send_x(r):
        return remote(latent, x_rows(tp), xs_sem.at[r], xr_sem.at[tp], tp=lax.rem(tp + r, n_tp))

    def recv_x(r):
        peer = lax.rem(tp + r, n_tp)
        return remote(latent, x_rows(peer), xs_sem.at[r], xr_sem.at[peer], tp=peer)

    for r in range(1, n_tp):
        send_x(r).start()

    loads[0].wait()
    stats_pass(context, cstat, ctx)

    total_mod = part[...]

    def add_a(r, acc):
        recv_a(r).wait_recv()
        return acc + part_a[lax.rem(sp + r, n_sp)]

    total_mod = lax.fori_loop(1, n_sp, add_a, total_mod)
    modbuf[tp] = total_mod

    def send_b(r):
        return remote(modbuf.at[tp], modbuf.at[tp], bs_sem.at[r], br_sem.at[tp], tp=lax.rem(tp + r, n_tp))

    def recv_b(r):
        peer = lax.rem(tp + r, n_tp)
        return remote(modbuf.at[peer], modbuf.at[peer], bs_sem.at[r], br_sem.at[peer], tp=peer)

    for r in range(1, n_tp):
        send_b(r).start()

    own_x.wait()
    for r in range(1, n_tp):
        recv_x(r).wait_recv()

    low = xbuf.at[pl.ds(0, EDGE)]
    high = xbuf.at[pl.ds(EDGE + tokens, EDGE)]
    first = xbuf.at[pl.ds(EDGE, EDGE)]
    last = xbuf.at[pl.ds(tokens, EDGE)]
    right = lax.rem(sp + 1, n_sp)
    left = lax.rem(sp + n_sp - 1, n_sp)
    to_right = remote(last, low, hs_sem.at[0], hr_sem.at[0], sp=right)
    to_left = remote(first, high, hs_sem.at[1], hr_sem.at[1], sp=left)
    has_right = sp < n_sp - 1
    has_left = sp > 0

    @pl.when(has_right)
    def _():
        to_right.start()

    @pl.when(has_left)
    def _():
        to_left.start()

    @pl.when(jnp.logical_not(has_left))
    def _():
        low[...] = jnp.zeros((EDGE, width), BF16)

    @pl.when(jnp.logical_not(has_right))
    def _():
        high[...] = jnp.zeros((EDGE, width), BF16)

    @pl.when(has_left)
    def _():
        to_right.wait_recv()

    @pl.when(has_right)
    def _():
        to_left.wait_recv()

    stats_pass(xbuf, xstat, tokens + 2 * EDGE)

    for r in range(1, n_tp):
        recv_b(r).wait_recv()
    mod = jnp.concatenate([modbuf[t] for t in range(n_tp)], axis=1)
    gain_l = norm_gain[...] * (1.0 + mod[1:2])
    shift_l = mod[0:1]
    gain_c = norm_gain[...] * (1.0 + mod[4:5])
    shift_c = mod[3:4]

    norm_pass(xbuf, xstat, hbuf, 0, 0, tokens + 2 * EDGE, gain_l, shift_l)

    for c in loads[1:5]:
        c.wait()
    hidden = hbuf[...]
    span = tokens + 2 * EDGE
    row_id = lax.broadcasted_iota(jnp.int32, (span, 1), 0)
    inside = jnp.logical_and(
        jnp.logical_or(row_id >= EDGE, has_left), jnp.logical_or(row_id < EDGE + tokens, has_right)
    )

    def rounded(x):
        return x.astype(BF16).astype(F32)

    ubuf[:, 0:vwidth] = jnp.where(inside, rounded(dotf(hidden, value_w[...])), 0.0)
    ubuf[:, vwidth : vwidth + mwidth] = jnp.where(inside, rounded(dotf(hidden, write_w[...])), 0.0)
    ubuf[:, vwidth + mwidth :] = jnp.where(inside, rounded(dotf(hidden, read_w[...])), 0.0)
    main = hbuf[EDGE : EDGE + tokens, :]

    def conv(ref, at, count, lo, hi, tap_lo):
        t = taps[:, tap_lo : tap_lo + hi - lo]
        return silu(
            t[0:1] * ref[pl.ds(at - 1, count), lo:hi]
            + t[1:2] * ref[pl.ds(at, count), lo:hi]
            + t[2:3] * ref[pl.ds(at + 1, count), lo:hi]
        )

    nrow = 2 * heads
    values = conv(ubuf, EDGE, tokens, 0, vwidth, 0)
    writes = conv(ubuf, EDGE, tokens, vwidth, vwidth + mwidth, vwidth)
    reads = conv(ubuf, EDGE, tokens, vwidth + mwidth, vwidth + 2 * mwidth, vwidth + mwidth)
    writes_b = writes.astype(BF16)
    reads_b = reads.astype(BF16)

    size = softplus(rounded(dot_nt(step[...], main)))[:nrow]
    decay = -size * rate[...] + jump[...]
    forward = lax.broadcasted_iota(jnp.int32, (nrow, 1), 0) < heads
    upto = tri_of(CHUNK, lambda k, i: k <= i)
    since = tri_of(CHUNK, lambda k, i: k >= i)
    after = tri_of(CHUNK, lambda k, i: k > i)
    before = tri_of(CHUNK, lambda k, i: k < i)
    cum = jnp.where(forward, dot32(decay, upto), dot32(decay, since))
    rest = jnp.where(forward, dot32(decay, after), dot32(decay, before))
    total = jnp.sum(decay, axis=1, keepdims=True)
    cols = columns_of(jnp.concatenate([cum, size * jnp.exp(rest), jnp.exp(cum)], axis=0))

    lane = lax.broadcasted_iota(jnp.int32, (1, gwidth), 1) // HEAD_DIM

    def by_head(pick, g):
        out_v = pick(g * per)
        for k in range(1, per):
            out_v = jnp.where(lane == k, pick(g * per + k), out_v)
        return out_v

    def states(write_t, vals, col_at, d):
        parts = []
        for g in range(groups):
            scale = by_head(lambda h: col_at(d * heads + h), g)
            scaled = (vals[:, g * gwidth : (g + 1) * gwidth] * scale).astype(BF16)
            parts.append(dotf(write_t, scaled)[g * STATE : (g + 1) * STATE])
        return jnp.concatenate(parts, axis=0)

    write_t = writes.T.astype(BF16)
    pad_rows = stbuf.shape[1] - mwidth - 2 * groups
    for d in range(2):
        st = states(write_t, values, lambda r: cols[:, nrow + r : nrow + r + 1], d)
        tot = jnp.concatenate(
            [by_head(lambda h: total[d * heads + h : d * heads + h + 1], g) for g in range(groups)], axis=0
        )
        tot_hi = tot.astype(BF16).astype(F32)
        extra = jnp.concatenate([tot_hi, tot - tot_hi, jnp.zeros((pad_rows, gwidth), F32)], axis=0)
        stbuf[d] = jnp.concatenate([st, extra], axis=0).astype(BF16)

    def send_s(d, k):
        return remote(stbuf.at[d], strecv.at[sp], ss_sem.at[k], sr_sem.at[sp], sp=k)

    def recv_s(k):
        return remote(stbuf.at[0], strecv.at[k], ss_sem.at[k], sr_sem.at[k], sp=k)

    @pl.loop(sp + 1, n_sp)
    def _(k):
        send_s(0, k).start()

    @pl.loop(0, sp)
    def _(k):
        send_s(1, k).start()

    pad8 = jnp.zeros((8, vwidth + mwidth), F32)
    ucbuf[0:8, :] = pad8
    ucbuf[8 + ctx : 16 + ctx, :] = pad8

    for i in range(ctx // CHUNK):
        norm_pass(context, cstat, chid, i * CHUNK, 0, CHUNK, gain_c, shift_c)
        hid = chid[...]
        ucbuf[8 + i * CHUNK : 8 + (i + 1) * CHUNK, 0:vwidth] = rounded(dotf(hid, value_w[...]))
        ucbuf[8 + i * CHUNK : 8 + (i + 1) * CHUNK, vwidth:] = rounded(dotf(hid, write_w[...]))
        cstep[i] = softplus(rounded(dot_nt(step[...], hid)))[:nrow]

    n_chunk = ctx // CHUNK
    decays = [-cstep[i] * rate[...] for i in range(n_chunk)]
    totals = [jnp.sum(a, axis=1, keepdims=True) for a in decays]
    entering = [None, None]
    for i in range(n_chunk):
        zero = jnp.zeros((nrow, 1), F32)
        later = sum(totals[i + 1 :], zero)
        earlier = sum(totals[:i], zero)
        rest_c = jnp.where(
            forward, dot32(decays[i], after) + later, dot32(decays[i], before) + earlier
        )
        ccols = columns_of(cstep[i] * jnp.exp(rest_c))
        cvals = conv(ucbuf, 8 + i * CHUNK, CHUNK, 0, vwidth, 0)
        cwrite_t = conv(ucbuf, 8 + i * CHUNK, CHUNK, vwidth, vwidth + mwidth, vwidth).T.astype(BF16)
        for d in range(2):
            st = states(cwrite_t, cvals, lambda r: ccols[:, r : r + 1], d)
            entering[d] = st if entering[d] is None else entering[d] + st

    ge = mask_of((tokens, tokens), lambda i, j: i >= j)
    le = mask_of((tokens, tokens), lambda i, j: i <= j)
    lane_m = lax.broadcasted_iota(jnp.int32, (1, mwidth), 1) // STATE
    inner = []
    for g in range(groups):
        own = jnp.where(lane_m == g, reads, 0.0).astype(BF16)
        score = dot_nt(own, writes_b)
        vg = values[:, g * gwidth : (g + 1) * gwidth].astype(BF16)
        made = []
        for k in range(per):
            h = g * per + k
            mix = jnp.zeros((tokens, tokens), F32)
            for d, keep in ((0, ge), (1, le)):
                r = d * heads + h
                gap = jnp.minimum(cols[:, r : r + 1] - cum[r : r + 1, :], 0.0)
                mix = mix + jnp.where(keep, jnp.exp(gap) * size[r : r + 1, :], 0.0)
            made.append(dotf((score * mix).astype(BF16), vg))
        inner.append(by_head(lambda h: made[h - g * per], g))
    mixer = skip[...] * values + jnp.concatenate(inner, axis=1)

    loads[5].wait()
    gate = silu(rounded(dotf(main, gate_w[...])))

    def join(k, state):
        recv_s(k).wait_recv()
        got = strecv[k].astype(F32)
        logs = got[mwidth : mwidth + groups] + got[mwidth + groups : mwidth + 2 * groups]
        fade = jnp.exp(logs)
        fade = jnp.concatenate(
            [jnp.broadcast_to(fade[g : g + 1], (STATE, gwidth)) for g in range(groups)], axis=0
        )
        return fade * state + got[:mwidth]

    entering[0] = lax.fori_loop(0, sp, join, entering[0])
    entering[1] = lax.fori_loop(0, n_sp - 1 - sp, lambda i, s: join(n_sp - 1 - i, s), entering[1])
    row_m = lax.broadcasted_iota(jnp.int32, (mwidth, 1), 0) // STATE
    for d in range(2):
        full = jnp.concatenate(
            [jnp.where(row_m == g, entering[d], 0.0) for g in range(groups)], axis=1
        ).astype(BF16)
        fade = jnp.concatenate(
            [
                by_head(lambda h: cols[:, 2 * nrow + d * heads + h : 2 * nrow + d * heads + h + 1], g)
                for g in range(groups)
            ],
            axis=1,
        )
        mixer = mixer + fade * dotf(reads_b, full)

    gated = mixer * gate
    pieces = []
    for g in range(groups):
        p = gated[:, g * gwidth : (g + 1) * gwidth]
        pieces.append(p * lax.rsqrt(jnp.mean(p * p, axis=-1, keepdims=True) + EPSILON))
    gated = (jnp.concatenate(pieces, axis=1) * group_gain[...]).astype(BF16)

    def send_o(c, r):
        peer = lax.rem(tp + r, n_tp)
        return remote(obuf.at[c, peer], rbuf.at[c, tp], os_sem.at[c, r], or_sem.at[c, tp], tp=peer)

    def recv_o(c, r):
        peer = lax.rem(tp + r, n_tp)
        return remote(obuf.at[c, peer], rbuf.at[c, peer], os_sem.at[c, r], or_sem.at[c, peer], tp=peer)

    for c in range(col_chunks):
        prod = dotf(gated, output_w[:, c * cwidth : (c + 1) * cwidth]).astype(BF16)
        for t in range(n_tp):
            obuf[c, t] = prod[t * rows : (t + 1) * rows]
        for r in range(1, n_tp):
            send_o(c, r).start()

    mixed = []
    for c in range(col_chunks):
        acc = obuf[c, tp].astype(F32)
        for r in range(1, n_tp):
            recv_o(c, r).wait_recv()
            acc = acc + rbuf[c, lax.rem(tp + r, n_tp)].astype(F32)
        mixed.append(acc)
    mixed = jnp.concatenate(mixed, axis=1)
    inv = lax.rsqrt(jnp.mean(mixed * mixed, axis=-1, keepdims=True) + EPSILON)
    gate_row = jnp.concatenate([modbuf[t, 2:3] for t in range(n_tp)], axis=1)
    out[...] = (latent[...].astype(F32) + gate_row * (mixed * inv * post_gain[...])).astype(BF16)

    @pl.loop(1, n_sp)
    def _(r):
        send_a(r).wait_send()

    for r in range(1, n_tp):
        send_x(r).wait_send()
        send_b(r).wait_send()

    @pl.when(has_right)
    def _():
        to_right.wait_send()

    @pl.when(has_left)
    def _():
        to_left.wait_send()

    @pl.loop(sp + 1, n_sp)
    def _(k):
        send_s(0, k).wait_send()

    @pl.loop(0, sp)
    def _(k):
        send_s(1, k).wait_send()

    for c in range(col_chunks):
        for r in range(1, n_tp):
            send_o(c, r).wait_send()


def body(
    latent, context, condition, context_condition, modulation_weight, norm_gain, gate_weight,
    value_weight, write_weight, read_weight, step_weight, value_taps, map_taps, decay_rate,
    decay_jump, skip_gain, group_gain, output_weight, post_gain,
):
    n_sp, n_tp = lax.axis_size("sp"), lax.axis_size("tp")
    sp, tp = lax.axis_index("sp"), lax.axis_index("tp")
    rows, width = latent.shape
    ctx = context.shape[0]
    vwidth, mwidth = value_weight.shape[1], write_weight.shape[1]
    heads, groups = vwidth // HEAD_DIM, mwidth // STATE
    gwidth = vwidth // groups
    tokens = rows * n_tp
    own_rows = modulation_weight.shape[0]
    share = modulation_weight.shape[2]
    conditions = jax.nn.silu(jnp.stack([condition, context_condition]))
    own = lax.dynamic_slice_in_dim(conditions, sp * own_rows, own_rows, 1)
    part = jnp.einsum("sd,dkc->skc", own, modulation_weight.astype(F32), precision=HIGHEST)
    part = jnp.pad(part.reshape(6, share), ((0, 2), (0, 0)))
    head_at = tp * heads
    nrow = 2 * heads
    step = lax.dynamic_slice_in_dim(step_weight, head_at, heads, 2)
    step = step.transpose(1, 2, 0).reshape(nrow, width)
    step = jnp.pad(step, ((0, -nrow % 16), (0, 0)))
    rate = lax.dynamic_slice_in_dim(decay_rate, head_at, heads, 1).reshape(nrow, 1)
    skip = jnp.repeat(lax.dynamic_slice_in_dim(skip_gain, head_at, heads, 0), HEAD_DIM).reshape(1, vwidth)
    taps = jnp.concatenate([value_taps, map_taps.reshape(3, -1)], axis=1).astype(F32)
    jump = decay_jump.reshape(nrow, tokens)
    chunks = 4
    cwidth = width // chunks
    srow = mwidth + 16
    vm = pltpu.VMEM
    dma = pltpu.SemaphoreType.DMA
    in_vmem = pl.BlockSpec(memory_space=pltpu.VMEM)
    in_any = pl.BlockSpec(memory_space=pl.ANY)
    return pl.pallas_call(
        functools.partial(kernel, n_sp=n_sp, n_tp=n_tp),
        out_shape=jax.ShapeDtypeStruct((rows, width), BF16),
        in_specs=[
            in_vmem, in_vmem, in_any, in_vmem, in_vmem, in_any, in_any, in_any, in_any,
            in_vmem, in_vmem, in_vmem, in_vmem, in_vmem, in_vmem, in_any,
        ],
        out_specs=in_vmem,
        scratch_shapes=[
            vm((ctx, width), BF16), vm((width, vwidth), BF16), vm((width, vwidth), BF16),
            vm((width, mwidth), BF16), vm((width, mwidth), BF16), vm((vwidth, width), BF16),
            vm((tokens + 2 * EDGE, width), BF16), vm((tokens + 2 * EDGE, 128), F32),
            vm((ctx, 128), F32), vm((tokens + 2 * EDGE, width), BF16), vm((CHUNK, width), BF16),
            vm((tokens + 2 * EDGE, vwidth + 2 * mwidth), F32), vm((ctx + 16, vwidth + mwidth), F32),
            vm((ctx // CHUNK, nrow, CHUNK), F32),
            vm((n_sp, 8, share), F32), vm((n_tp, 8, share), F32),
            vm((2, srow, gwidth), BF16), vm((n_sp, srow, gwidth), BF16),
            vm((chunks, n_tp, rows, cwidth), BF16), vm((chunks, n_tp, rows, cwidth), BF16),
            vm((2, mwidth, gwidth), F32),
            dma((6,)), dma, dma((n_tp,)), dma((n_tp,)), dma((2,)), dma((2,)),
            dma((n_sp,)), dma((n_sp,)), dma((n_tp,)), dma((n_tp,)), dma((n_sp,)), dma((n_sp,)),
            dma((chunks, n_tp)), dma((chunks, n_tp)),
        ],
        compiler_params=pltpu.CompilerParams(
            collective_id=0, has_side_effects=True, vmem_limit_bytes=48 * 1024 * 1024
        ),
    )(
        part, latent, context, norm_gain.reshape(1, -1), post_gain.reshape(1, -1), gate_weight,
        value_weight, write_weight, read_weight, step, taps, rate, jump, skip,
        group_gain.reshape(1, -1), output_weight,
    )


def solution(mesh):
    placed = (
        P(("sp", "tp"), None), P(), P(), P(), P("sp", None, "tp"), P(), P(None, "tp"), P(None, "tp"),
        P(None, "tp"), P(None, "tp"), P(), P(None, "tp"), P(None, None, "tp"), P(),
        P(None, "tp", "sp"), P(), P("tp"), P("tp", None), P(),
    )
    return jax.shard_map(
        body, mesh=mesh, in_specs=placed, out_specs=P(("sp", "tp"), None), check_vma=False
    )
```

```python
import functools

import jax
import jax.numpy as jnp
from jax import lax
from jax.experimental import pallas as pl
from jax.experimental.pallas import tpu as pltpu
from jax.sharding import PartitionSpec as P

HEAD_DIM = 64
STATE = 64
EPSILON = 1e-06
HIGHEST = lax.Precision.HIGHEST
MESH = pl.DeviceIdType.MESH
EDGE = 16
CHUNK = 128
F32 = jnp.float32
BF16 = jnp.bfloat16


def silu(x):
    return x / (1.0 + jnp.exp(-x))


def softplus(x):
    return jnp.maximum(x, 0.0) + jnp.log1p(jnp.exp(-jnp.abs(x)))


def mask_of(shape, rule):
    rows = lax.broadcasted_iota(jnp.int32, shape, 0)
    cols = lax.broadcasted_iota(jnp.int32, shape, 1)
    return rule(rows, cols)


def tri_of(size, rule):
    return jnp.where(mask_of((size, size), rule), 1.0, 0.0).astype(F32)


def dot32(a, b):
    return jnp.dot(a, b, precision=HIGHEST, preferred_element_type=F32)


def dotf(a, b):
    return jnp.dot(a, b, preferred_element_type=F32)


def dot_nt(a, b):
    return lax.dot_general(a, b, (((1,), (1,)), ((), ())), preferred_element_type=F32)


def columns_of(rows8):
    have = rows8.shape[0]
    pad = jnp.zeros((CHUNK - have, CHUNK), F32)
    return jnp.concatenate([rows8, pad], axis=0).T


def stats_pass(src, dst, count):
    @pl.loop(0, count // 16)
    def _(i):
        at = pl.ds(pl.multiple_of(i * 16, 16), 16)
        x = src[at, :].astype(F32)
        inv = lax.rsqrt(jnp.mean(x * x, axis=-1, keepdims=True) + EPSILON)
        dst[at, :] = jnp.broadcast_to(inv, (16, 128))


def norm_pass(src, stat, dst, src_at, dst_at, count, gain, shift):
    lanes = src.shape[1] // 128

    @pl.loop(0, count // 16)
    def _(i):
        at = pl.ds(pl.multiple_of(src_at + i * 16, 16), 16)
        to = pl.ds(pl.multiple_of(dst_at + i * 16, 16), 16)
        inv = jnp.concatenate([stat[at, :]] * lanes, axis=1)
        dst[to, :] = (src[at, :].astype(F32) * inv * gain + shift).astype(BF16)


def kernel(
    latent_hbm, context_hbm, cond_hbm, ccond_hbm, mod_hbm, norm_hbm, gate_hbm, value_hbm,
    write_hbm, read_hbm, step_hbm, vtaps_hbm, mtaps_hbm, rate_hbm, jump_hbm, skip_hbm,
    ggain_hbm, output_hbm, post_hbm,
    out,
    context, gate_w, value_w, write_w, read_w, output_w,
    cond, ccond, mod_w, norm_gain, step, vtaps, mtaps, rate_v, jump, skip_v, group_gain, post_gain,
    part, picked,
    xbuf, xstat, cstat, hbuf, chid, ubuf, ucbuf, cstep,
    part_a, modbuf, stbuf, strecv, obuf, rbuf, state_c,
    load_sem, own_sem, xs_sem, xr_sem, hs_sem, hr_sem, as_sem, ar_sem, bs_sem, br_sem,
    ss_sem, sr_sem, os_sem, or_sem,
    *, n_sp, n_tp, sliced,
):
    sp, tp = lax.axis_index("sp"), lax.axis_index("tp")
    rows = latent_hbm.shape[0]
    tokens = n_tp * rows
    width = latent_hbm.shape[1]
    vwidth = value_w.shape[1]
    mwidth = write_w.shape[1]
    groups = mwidth // STATE
    heads = vwidth // HEAD_DIM
    per = heads // groups
    gwidth = vwidth // groups
    ctx = context.shape[0]
    col_chunks = obuf.shape[0]
    cwidth = obuf.shape[3]

    loads = [
        pltpu.make_async_copy(s, d, load_sem.at[i])
        for i, (s, d) in enumerate(
            (
                (mod_hbm, mod_w), (cond_hbm, cond), (ccond_hbm, ccond), (context_hbm, context),
                (norm_hbm, norm_gain), (value_hbm, value_w), (write_hbm, write_w),
                (read_hbm, read_w), (step_hbm, step), (vtaps_hbm, vtaps), (mtaps_hbm, mtaps),
                (rate_hbm, rate_v), (jump_hbm, jump), (skip_hbm, skip_v), (gate_hbm, gate_w),
                (output_hbm, output_w), (ggain_hbm, group_gain), (post_hbm, post_gain),
            )
        )
    ]
    mine = pl.ds(pl.multiple_of(EDGE + tp * rows, 16), rows)
    latent = xbuf.at[mine]
    own_x = pltpu.make_async_copy(latent_hbm, latent, own_sem)
    own_x.start()
    for c in loads:
        c.start()

    barrier = pltpu.get_barrier_semaphore()

    @pl.loop(1, n_sp)
    def _(r):
        pl.semaphore_signal(barrier, inc=1, device_id={"sp": lax.rem(sp + r, n_sp)}, device_id_type=MESH)

    for r in range(1, n_tp):
        pl.semaphore_signal(barrier, inc=1, device_id={"tp": lax.rem(tp + r, n_tp)}, device_id_type=MESH)
    pl.semaphore_wait(barrier, n_sp - 1 + n_tp - 1)

    def remote(src, dst, s, r, **where):
        return pltpu.make_async_remote_copy(
            src_ref=src, dst_ref=dst, send_sem=s, recv_sem=r, device_id=where, device_id_type=MESH
        )

    own_x.wait()

    def x_rows(t):
        return xbuf.at[pl.ds(pl.multiple_of(EDGE + t * rows, 16), rows)]

    def send_x(r):
        return remote(latent, x_rows(tp), xs_sem.at[r], xr_sem.at[tp], tp=lax.rem(tp + r, n_tp))

    def recv_x(r):
        peer = lax.rem(tp + r, n_tp)
        return remote(latent, x_rows(peer), xs_sem.at[r], xr_sem.at[peer], tp=peer)

    for r in range(1, n_tp):
        send_x(r).start()

    for c in loads[0:3]:
        c.wait()
    depth = mod_w.shape[1]
    if sliced:
        own = pl.ds(0, depth)
    else:
        own = pl.ds(pl.multiple_of(sp * depth, 128), depth)
    left_over = [silu(cond[:, own]), silu(ccond[:, own])]
    split = []
    for _ in range(3):
        for v in range(2):
            high = left_over[v].astype(BF16).astype(F32)
            split.append(high)
            left_over[v] = left_over[v] - high
    split.append(jnp.zeros((10, depth), F32))
    split = jnp.concatenate(split, axis=0).astype(BF16)
    prods = [dotf(split, mod_w[k]) for k in range(3)]
    lines = [p[v : v + 1] + p[v + 2 : v + 3] + p[v + 4 : v + 5] for v in range(2) for p in prods]
    lines.append(jnp.zeros((2, part.shape[1]), F32))
    part[...] = jnp.concatenate(lines, axis=0)

    def send_a(r):
        peer = lax.rem(sp + r, n_sp)
        return remote(part, part_a.at[sp], as_sem.at[r], ar_sem.at[sp], sp=peer)

    def recv_a(r):
        peer = lax.rem(sp + r, n_sp)
        return remote(part, part_a.at[peer], as_sem.at[r], ar_sem.at[peer], sp=peer)

    @pl.loop(1, n_sp)
    def _(r):
        send_a(r).start()

    loads[3].wait()
    stats_pass(context, cstat, ctx)

    total_mod = part[...]

    def add_a(r, acc):
        recv_a(r).wait_recv()
        return acc + part_a[lax.rem(sp + r, n_sp)]

    total_mod = lax.fori_loop(1, n_sp, add_a, total_mod)
    modbuf[tp] = total_mod

    def send_b(r):
        return remote(modbuf.at[tp], modbuf.at[tp], bs_sem.at[r], br_sem.at[tp], tp=lax.rem(tp + r, n_tp))

    def recv_b(r):
        peer = lax.rem(tp + r, n_tp)
        return remote(modbuf.at[peer], modbuf.at[peer], bs_sem.at[r], br_sem.at[peer], tp=peer)

    for r in range(1, n_tp):
        send_b(r).start()

    for r in range(1, n_tp):
        recv_x(r).wait_recv()

    low = xbuf.at[pl.ds(0, EDGE)]
    high = xbuf.at[pl.ds(EDGE + tokens, EDGE)]
    first = xbuf.at[pl.ds(EDGE, EDGE)]
    last = xbuf.at[pl.ds(tokens, EDGE)]
    right = lax.rem(sp + 1, n_sp)
    left = lax.rem(sp + n_sp - 1, n_sp)
    to_right = remote(last, low, hs_sem.at[0], hr_sem.at[0], sp=right)
    to_left = remote(first, high, hs_sem.at[1], hr_sem.at[1], sp=left)
    has_right = sp < n_sp - 1
    has_left = sp > 0

    @pl.when(has_right)
    def _():
        to_right.start()

    @pl.when(has_left)
    def _():
        to_left.start()

    @pl.when(jnp.logical_not(has_left))
    def _():
        low[...] = jnp.zeros((EDGE, width), BF16)

    @pl.when(jnp.logical_not(has_right))
    def _():
        high[...] = jnp.zeros((EDGE, width), BF16)

    @pl.when(has_left)
    def _():
        to_right.wait_recv()

    @pl.when(has_right)
    def _():
        to_left.wait_recv()

    stats_pass(xbuf, xstat, tokens + 2 * EDGE)

    for r in range(1, n_tp):
        recv_b(r).wait_recv()
    loads[4].wait()
    mod = jnp.concatenate([modbuf[t] for t in range(n_tp)], axis=1)
    gain_l = norm_gain[...] * (1.0 + mod[1:2])
    shift_l = mod[0:1]
    gain_c = norm_gain[...] * (1.0 + mod[4:5])
    shift_c = mod[3:4]

    norm_pass(xbuf, xstat, hbuf, 0, 0, tokens + 2 * EDGE, gain_l, shift_l)

    for c in loads[5:14]:
        c.wait()
    hidden = hbuf[...]
    span = tokens + 2 * EDGE
    row_id = lax.broadcasted_iota(jnp.int32, (span, 1), 0)
    inside = jnp.logical_and(
        jnp.logical_or(row_id >= EDGE, has_left), jnp.logical_or(row_id < EDGE + tokens, has_right)
    )

    def rounded(x):
        return x.astype(BF16).astype(F32)

    ubuf[:, 0:vwidth] = jnp.where(inside, rounded(dotf(hidden, value_w[...])), 0.0)
    ubuf[:, vwidth : vwidth + mwidth] = jnp.where(inside, rounded(dotf(hidden, write_w[...])), 0.0)
    ubuf[:, vwidth + mwidth :] = jnp.where(inside, rounded(dotf(hidden, read_w[...])), 0.0)
    main = hbuf[EDGE : EDGE + tokens, :]

    def conv(ref, at, count, lo, hi, t):
        return silu(
            t[0] * ref[pl.ds(at - 1, count), lo:hi]
            + t[1] * ref[pl.ds(at, count), lo:hi]
            + t[2] * ref[pl.ds(at + 1, count), lo:hi]
        )

    value_t = [vtaps[i : i + 1, :].astype(F32) for i in range(3)]
    write_t3, read_t3 = ([mtaps[i, k : k + 1, :].astype(F32) for i in range(3)] for k in range(2))
    nrow = 2 * heads
    values = conv(ubuf, EDGE, tokens, 0, vwidth, value_t)
    writes = conv(ubuf, EDGE, tokens, vwidth, vwidth + mwidth, write_t3)
    reads = conv(ubuf, EDGE, tokens, vwidth + mwidth, vwidth + 2 * mwidth, read_t3)
    writes_b = writes.astype(BF16)
    reads_b = reads.astype(BF16)

    every = step.shape[0] // 2
    head_at = tp * heads

    def own_steps(hid):
        picked[...] = dot_nt(step[...], hid)
        rows_d = [picked[pl.ds(d * every + head_at, heads), :] for d in range(2)]
        return softplus(rounded(jnp.concatenate(rows_d, axis=0)))

    at_row = lax.broadcasted_iota(jnp.int32, (nrow, every), 0)
    at_lane = lax.broadcasted_iota(jnp.int32, (nrow, every), 1)
    rates = jnp.where(at_row < heads, rate_v[0:1, :], rate_v[1:2, :])
    rate = jnp.sum(
        jnp.where(at_lane == head_at + lax.rem(at_row, heads), rates, 0.0), axis=1, keepdims=True
    )
    head_of = lax.broadcasted_iota(jnp.int32, (1, vwidth), 1) // HEAD_DIM
    line = lax.broadcasted_iota(jnp.int32, (1, every), 1)
    skip = jnp.zeros((1, vwidth), F32)
    for h in range(heads):
        own_skip = jnp.sum(jnp.where(line == head_at + h, skip_v[...], 0.0), axis=1, keepdims=True)
        skip = jnp.where(head_of == h, own_skip, skip)
    size = own_steps(main)
    decay = -size * rate + jump[...]
    forward = lax.broadcasted_iota(jnp.int32, (nrow, 1), 0) < heads
    upto = tri_of(CHUNK, lambda k, i: k <= i)
    since = tri_of(CHUNK, lambda k, i: k >= i)
    after = tri_of(CHUNK, lambda k, i: k > i)
    before = tri_of(CHUNK, lambda k, i: k < i)
    cum = jnp.where(forward, dot32(decay, upto), dot32(decay, since))
    rest = jnp.where(forward, dot32(decay, after), dot32(decay, before))
    total = jnp.sum(decay, axis=1, keepdims=True)
    cols = columns_of(jnp.concatenate([cum, size * jnp.exp(rest), jnp.exp(cum)], axis=0))

    lane = lax.broadcasted_iota(jnp.int32, (1, gwidth), 1) // HEAD_DIM

    def by_head(pick, g):
        out_v = pick(g * per)
        for k in range(1, per):
            out_v = jnp.where(lane == k, pick(g * per + k), out_v)
        return out_v

    def states(write_t, vals, col_at, d):
        parts = []
        for g in range(groups):
            scale = by_head(lambda h: col_at(d * heads + h), g)
            scaled = (vals[:, g * gwidth : (g + 1) * gwidth] * scale).astype(BF16)
            parts.append(dotf(write_t, scaled)[g * STATE : (g + 1) * STATE])
        return jnp.concatenate(parts, axis=0)

    write_t = writes.T.astype(BF16)
    pad_rows = stbuf.shape[1] - mwidth - 2 * groups
    for d in range(2):
        st = states(write_t, values, lambda r: cols[:, nrow + r : nrow + r + 1], d)
        tot = jnp.concatenate(
            [by_head(lambda h: total[d * heads + h : d * heads + h + 1], g) for g in range(groups)], axis=0
        )
        tot_hi = tot.astype(BF16).astype(F32)
        extra = jnp.concatenate([tot_hi, tot - tot_hi, jnp.zeros((pad_rows, gwidth), F32)], axis=0)
        stbuf[d] = jnp.concatenate([st, extra], axis=0).astype(BF16)

    def send_s(d, k):
        return remote(stbuf.at[d], strecv.at[sp], ss_sem.at[k], sr_sem.at[sp], sp=k)

    def recv_s(k):
        return remote(stbuf.at[0], strecv.at[k], ss_sem.at[k], sr_sem.at[k], sp=k)

    @pl.loop(sp + 1, n_sp)
    def _(k):
        send_s(0, k).start()

    @pl.loop(0, sp)
    def _(k):
        send_s(1, k).start()

    pad8 = jnp.zeros((8, vwidth + mwidth), F32)
    ucbuf[0:8, :] = pad8
    ucbuf[8 + ctx : 16 + ctx, :] = pad8

    for i in range(ctx // CHUNK):
        norm_pass(context, cstat, chid, i * CHUNK, 0, CHUNK, gain_c, shift_c)
        hid = chid[...]
        ucbuf[8 + i * CHUNK : 8 + (i + 1) * CHUNK, 0:vwidth] = rounded(dotf(hid, value_w[...]))
        ucbuf[8 + i * CHUNK : 8 + (i + 1) * CHUNK, vwidth:] = rounded(dotf(hid, write_w[...]))
        cstep[i] = own_steps(hid)

    n_chunk = ctx // CHUNK
    decays = [-cstep[i] * rate for i in range(n_chunk)]
    totals = [jnp.sum(a, axis=1, keepdims=True) for a in decays]
    entering = [None, None]
    for i in range(n_chunk):
        zero = jnp.zeros((nrow, 1), F32)
        later = sum(totals[i + 1 :], zero)
        earlier = sum(totals[:i], zero)
        rest_c = jnp.where(
            forward, dot32(decays[i], after) + later, dot32(decays[i], before) + earlier
        )
        ccols = columns_of(cstep[i] * jnp.exp(rest_c))
        cvals = conv(ucbuf, 8 + i * CHUNK, CHUNK, 0, vwidth, value_t)
        cwrite_t = conv(ucbuf, 8 + i * CHUNK, CHUNK, vwidth, vwidth + mwidth, write_t3).T.astype(BF16)
        for d in range(2):
            st = states(cwrite_t, cvals, lambda r: ccols[:, r : r + 1], d)
            entering[d] = st if entering[d] is None else entering[d] + st

    ge = mask_of((tokens, tokens), lambda i, j: i >= j)
    le = mask_of((tokens, tokens), lambda i, j: i <= j)
    lane_m = lax.broadcasted_iota(jnp.int32, (1, mwidth), 1) // STATE
    inner = []
    for g in range(groups):
        own = jnp.where(lane_m == g, reads, 0.0).astype(BF16)
        score = dot_nt(own, writes_b)
        vg = values[:, g * gwidth : (g + 1) * gwidth].astype(BF16)
        made = []
        for k in range(per):
            h = g * per + k
            mix = jnp.zeros((tokens, tokens), F32)
            for d, keep in ((0, ge), (1, le)):
                r = d * heads + h
                gap = jnp.minimum(cols[:, r : r + 1] - cum[r : r + 1, :], 0.0)
                mix = mix + jnp.where(keep, jnp.exp(gap) * size[r : r + 1, :], 0.0)
            made.append(dotf((score * mix).astype(BF16), vg))
        inner.append(by_head(lambda h: made[h - g * per], g))
    mixer = skip * values + jnp.concatenate(inner, axis=1)

    for c in loads[14:]:
        c.wait()
    gate = silu(rounded(dotf(main, gate_w[...])))

    def join(k, state):
        recv_s(k).wait_recv()
        got = strecv[k].astype(F32)
        logs = got[mwidth : mwidth + groups] + got[mwidth + groups : mwidth + 2 * groups]
        fade = jnp.exp(logs)
        fade = jnp.concatenate(
            [jnp.broadcast_to(fade[g : g + 1], (STATE, gwidth)) for g in range(groups)], axis=0
        )
        return fade * state + got[:mwidth]

    entering[0] = lax.fori_loop(0, sp, join, entering[0])
    entering[1] = lax.fori_loop(0, n_sp - 1 - sp, lambda i, s: join(n_sp - 1 - i, s), entering[1])
    row_m = lax.broadcasted_iota(jnp.int32, (mwidth, 1), 0) // STATE
    for d in range(2):
        full = jnp.concatenate(
            [jnp.where(row_m == g, entering[d], 0.0) for g in range(groups)], axis=1
        ).astype(BF16)
        fade = jnp.concatenate(
            [
                by_head(lambda h: cols[:, 2 * nrow + d * heads + h : 2 * nrow + d * heads + h + 1], g)
                for g in range(groups)
            ],
            axis=1,
        )
        mixer = mixer + fade * dotf(reads_b, full)

    gated = mixer * gate
    pieces = []
    for g in range(groups):
        p = gated[:, g * gwidth : (g + 1) * gwidth]
        pieces.append(p * lax.rsqrt(jnp.mean(p * p, axis=-1, keepdims=True) + EPSILON))
    gated = (jnp.concatenate(pieces, axis=1) * group_gain[...]).astype(BF16)

    def send_o(c, r):
        peer = lax.rem(tp + r, n_tp)
        return remote(obuf.at[c, peer], rbuf.at[c, tp], os_sem.at[c, r], or_sem.at[c, tp], tp=peer)

    def recv_o(c, r):
        peer = lax.rem(tp + r, n_tp)
        return remote(obuf.at[c, peer], rbuf.at[c, peer], os_sem.at[c, r], or_sem.at[c, peer], tp=peer)

    for c in range(col_chunks):
        prod = dotf(gated, output_w[:, c * cwidth : (c + 1) * cwidth]).astype(BF16)
        for t in range(n_tp):
            obuf[c, t] = prod[t * rows : (t + 1) * rows]
        for r in range(1, n_tp):
            send_o(c, r).start()

    mixed = []
    for c in range(col_chunks):
        acc = obuf[c, tp].astype(F32)
        for r in range(1, n_tp):
            recv_o(c, r).wait_recv()
            acc = acc + rbuf[c, lax.rem(tp + r, n_tp)].astype(F32)
        mixed.append(acc)
    mixed = jnp.concatenate(mixed, axis=1)
    inv = lax.rsqrt(jnp.mean(mixed * mixed, axis=-1, keepdims=True) + EPSILON)
    gate_row = jnp.concatenate([modbuf[t, 2:3] for t in range(n_tp)], axis=1)
    out[...] = (latent[...].astype(F32) + gate_row * (mixed * inv * post_gain[...])).astype(BF16)

    @pl.loop(1, n_sp)
    def _(r):
        send_a(r).wait_send()

    for r in range(1, n_tp):
        send_x(r).wait_send()
        send_b(r).wait_send()

    @pl.when(has_right)
    def _():
        to_right.wait_send()

    @pl.when(has_left)
    def _():
        to_left.wait_send()

    @pl.loop(sp + 1, n_sp)
    def _(k):
        send_s(0, k).wait_send()

    @pl.loop(0, sp)
    def _(k):
        send_s(1, k).wait_send()

    for c in range(col_chunks):
        for r in range(1, n_tp):
            send_o(c, r).wait_send()


def body(
    latent, context, condition, context_condition, modulation_weight, norm_gain, gate_weight,
    value_weight, write_weight, read_weight, step_weight, value_taps, map_taps, decay_rate,
    decay_jump, skip_gain, group_gain, output_weight, post_gain,
):
    n_sp, n_tp = lax.axis_size("sp"), lax.axis_size("tp")
    sp, tp = lax.axis_index("sp"), lax.axis_index("tp")
    rows, width = latent.shape
    ctx = context.shape[0]
    vwidth, mwidth = value_weight.shape[1], write_weight.shape[1]
    heads, groups = vwidth // HEAD_DIM, mwidth // STATE
    gwidth = vwidth // groups
    tokens = rows * n_tp
    own_rows = modulation_weight.shape[0]
    share = modulation_weight.shape[2]
    nrow = 2 * heads
    conds = [condition.reshape(1, -1), context_condition.reshape(1, -1)]
    sliced = own_rows % 128 != 0
    if sliced:
        conds = [lax.dynamic_slice_in_dim(c, sp * own_rows, own_rows, 1) for c in conds]
    every = decay_rate.shape[1]
    chunks = 4
    cwidth = width // chunks
    srow = mwidth + 16
    vm = pltpu.VMEM
    dma = pltpu.SemaphoreType.DMA
    in_vmem = pl.BlockSpec(memory_space=pltpu.VMEM)
    in_any = pl.BlockSpec(memory_space=pl.ANY)
    return pl.pallas_call(
        functools.partial(kernel, n_sp=n_sp, n_tp=n_tp, sliced=sliced),
        out_shape=jax.ShapeDtypeStruct((rows, width), BF16),
        in_specs=[in_any] * 19,
        out_specs=in_vmem,
        scratch_shapes=[
            vm((ctx, width), BF16), vm((width, vwidth), BF16), vm((width, vwidth), BF16),
            vm((width, mwidth), BF16), vm((width, mwidth), BF16), vm((vwidth, width), BF16),
            vm(conds[0].shape, F32), vm(conds[0].shape, F32), vm((3, own_rows, share), BF16),
            vm((1, width), F32), vm((2 * every, width), BF16), vm((3, vwidth), BF16),
            vm((3, 2, mwidth), BF16), vm((2, every), F32), vm((nrow, tokens), F32),
            vm((1, every), F32), vm((1, vwidth), F32), vm((1, width), F32),
            vm((8, share), F32), vm((2 * every, CHUNK), F32),
            vm((tokens + 2 * EDGE, width), BF16), vm((tokens + 2 * EDGE, 128), F32),
            vm((ctx, 128), F32), vm((tokens + 2 * EDGE, width), BF16), vm((CHUNK, width), BF16),
            vm((tokens + 2 * EDGE, vwidth + 2 * mwidth), F32), vm((ctx + 16, vwidth + mwidth), F32),
            vm((ctx // CHUNK, nrow, CHUNK), F32),
            vm((n_sp, 8, share), F32), vm((n_tp, 8, share), F32),
            vm((2, srow, gwidth), BF16), vm((n_sp, srow, gwidth), BF16),
            vm((chunks, n_tp, rows, cwidth), BF16), vm((chunks, n_tp, rows, cwidth), BF16),
            vm((2, mwidth, gwidth), F32),
            dma((18,)), dma, dma((n_tp,)), dma((n_tp,)), dma((2,)), dma((2,)),
            dma((n_sp,)), dma((n_sp,)), dma((n_tp,)), dma((n_tp,)), dma((n_sp,)), dma((n_sp,)),
            dma((chunks, n_tp)), dma((chunks, n_tp)),
        ],
        compiler_params=pltpu.CompilerParams(
            collective_id=0, has_side_effects=True, vmem_limit_bytes=62 * 1024 * 1024
        ),
    )(
        latent, context, *conds, modulation_weight.transpose(1, 0, 2), norm_gain.reshape(1, -1),
        gate_weight, value_weight, write_weight, read_weight,
        step_weight.transpose(1, 2, 0).reshape(2 * every, width), value_taps, map_taps, decay_rate,
        decay_jump.reshape(nrow, tokens), skip_gain.reshape(1, -1), group_gain.reshape(1, -1),
        output_weight, post_gain.reshape(1, -1),
    )


def solution(mesh):
    placed = (
        P(("sp", "tp"), None), P(), P(), P(), P("sp", None, "tp"), P(), P(None, "tp"), P(None, "tp"),
        P(None, "tp"), P(None, "tp"), P(), P(None, "tp"), P(None, None, "tp"), P(),
        P(None, "tp", "sp"), P(), P("tp"), P("tp", None), P(),
    )
    return jax.shard_map(
        body, mesh=mesh, in_specs=placed, out_specs=P(("sp", "tp"), None), check_vma=False
    )
```
